256 devices in a mesh: ep: 64 (over z, y, x_hi), tp: 4 (over x_lo, core).
Axes of the slice: x: 4 (x_hi: 2, x_lo: 2; x = x_hi * 2 + x_lo), y: 4, z: 8, core: 2. Of those that a mesh axis runs over, the one named last changes fastest.
Arguments:
- tokens: bfloat16 [1536, 1024], P('ep'), may hold values from -3 to 3
- attn_gain: float32 [1024], replicated, may hold values from 0.1 to 1.9
- w_query: bfloat16 [1024, 1024], P(None, 'tp'), may hold values from -0.1875 to 0.1875
- w_key: bfloat16 [1024, 256], P(None, 'tp'), may hold values from -0.1875 to 0.1875
- w_value: bfloat16 [1024, 256], P(None, 'tp'), may hold values from -0.1875 to 0.1875
- attn_bias: float32 [16], P('tp'), may hold values from -7.5 to -3
- key_cache: bfloat16 [1536, 256, 1024], P('ep', 'tp'), may hold values from -6 to 6
- value_cache: bfloat16 [1536, 256, 1024], P('ep', 'tp'), may hold values from -6 to 6
- lengths: int32 [1536], P('ep'), may hold values from 128 to 1024
- w_out: bfloat16 [1024, 1024], P('tp'), may hold values from -0.75 to 0.75
- ffn_gain: float32 [1024], replicated, may hold values from 0.1 to 1.9
- routes: int32 [1536, 2], P('ep'), may hold values from 0 to 63, all different within a row; in each aligned block of 24 rows (0 to 23, 24 to 47, ...) at most 2 rows name the same one
- route_weight: float32 [1536, 2], P('ep'), may hold values from 0.2 to 1
- expert_gate: bfloat16 [64, 1024, 3584], P('ep', None, 'tp'), may hold values from -0.1875 to 0.1875
- expert_up: bfloat16 [64, 1024, 3584], P('ep', None, 'tp'), may hold values from -0.1875 to 0.1875
- expert_down: bfloat16 [64, 3584, 1024], P('ep', 'tp'), may hold values from -0.09375 to 0.09375
Outputs:
- mixed: bfloat16 [1536, 1024], P('ep')
- new_keys: bfloat16 [1536, 256], P('ep', 'tp')
- new_values: bfloat16 [1536, 256], P('ep', 'tp')
The draws below stay inside these ranges and needn't reach their ends.
Inputs may be any that keep to these rules, and one draw needn't show every extreme that they name: `routes`: each row names 2 different experts. Among the rows of one device no expert is named by more than 2 of them, and on some device some expert is named by exactly 2.
All inputs are finite; a program needn't handle non-finite values.
Results may differ from the reference program's by a relative error of at most 0.02.
Values may be sent and summed in bfloat16 or wider, within the bound.
A program may use at most 64 MiB of HBM per device.

```python
import math
import jax
import jax.numpy as jnp
import numpy as np
from jax import lax

D = 1024
HEADS = 16
KV_HEADS = 4
HEAD = 64
FF = 3584
TOP = 2
SEQS = 24
LEN = 1024
EXPERTS = 64
CAP = 2
BATCH = 1536
N_EP = 64
N_TP = 4


def set_ends(drawn, stream_key, least, top_value):
    dims = drawn.shape
    index_at = [jax.random.randint(jax.random.fold_in(stream_key, axis), (), 0, dims[axis]) for axis in range(len(dims))]
    drawn = drawn.at[tuple(index_at)].set(least)
    longest = dims.index(max(dims))
    index_at[longest] = (index_at[longest] + 1) % dims[longest]
    return drawn.at[tuple(index_at)].set(top_value)


def level_of(stream_key, dims, cuts, low, high):
    def one(dim, shards_of):
        steps = jax.random.uniform(jax.random.fold_in(jax.random.fold_in(stream_key, 6), dim), (shards_of,), jnp.float32, low / len(cuts), high / len(cuts))
        return jnp.repeat(jnp.exp(steps), dims[dim] // shards_of).reshape((-1,) + (1,) * (len(dims) - dim - 1))

    factor_of = one(*cuts[0])
    for cut in cuts[1:]:
        factor_of = factor_of * one(*cut)
    return factor_of


def routed_block(rng, own, number, rows, number_of, top, limit, lean):
    order = jax.random.permutation(rng, number_of)
    heavy_load, usual = shares(number_of, rows * top, limit, lean, True), shares(number_of, rows * top, limit, lean, False)
    places = jnp.arange(number_of)

    def named(sizes, offset_by):
        used = int((sizes > 0).sum())
        fixed = max(1, used // 4)
        passed = fixed + (places - fixed + offset_by * (used - fixed)) % max(1, number_of - fixed)
        return jnp.zeros((number_of,), jnp.int32).at[order[jnp.where(places < fixed, places, passed)]].set(jnp.asarray(sizes, jnp.int32))

    sizes = jnp.where(number % 4 == 0, named(heavy_load, number // 4), named(usual, number - number // 4 - 1))
    mixed = jax.random.permutation(jax.random.fold_in(own, 3), number_of)
    donor, sink = mixed[0:number_of // 2 * 2:2], mixed[1:number_of // 2 * 2:2]
    margin = jnp.minimum(sizes[donor] - 1, limit - sizes[sink]) // 2
    margin = jnp.where((donor == order[0]) | (sink == order[0]) | (sizes[sink] == 0), 0, jnp.maximum(margin, 0))
    passed = jax.random.randint(jax.random.fold_in(own, 4), (number_of // 2,), 0, 1 << 20) % (margin + 1)
    sizes = sizes.at[donor].add(-passed).at[sink].add(passed)
    labels = jnp.searchsorted(jnp.cumsum(sizes), jnp.arange(rows * top), side="right").astype(jnp.int32)
    grid = labels.reshape(top, rows).T
    grid = grid[jax.random.permutation(jax.random.fold_in(own, 1), rows)]
    offset_by = jax.random.randint(jax.random.fold_in(own, 2), (rows, 1), 0, top)
    return jnp.take_along_axis(grid, (jnp.arange(top)[None, :] + offset_by) % top, axis=1)


def shares(amount, total, bound, skew, full):
    portions = [(1 << 20) // math.isqrt(rank ** skew) + 1 for rank in range(1, amount + 1)]
    largest = bound if full else min(bound, max(-(-total // amount), total * portions[0] // sum(portions)))
    least = 1 if total - largest >= amount - 1 else 0
    given, surplus = [largest] + [least] * (amount - 1), total - largest - least * (amount - 1)
    while surplus > 0:
        movable = [i for i in range(1, amount) if given[i] < largest] or [i for i in range(1, amount) if given[i] < bound]
        whole, remaining = sum([portions[i] for i in movable]), surplus
        for i in movable:
            extra = min(bound - given[i], max(1, remaining * portions[i] // whole), surplus)
            given[i] = given[i] + extra
            surplus = surplus - extra
    return np.array(given)


def normal_values(key, shape, scale, most, shards=(), kind=jnp.bfloat16):
    array = scale * jax.random.normal(key, shape, jnp.float32)
    if shards:
        array = array * level_of(key, shape, shards, -0.22, 0.18)
    return jnp.clip(array, -most, most).astype(kind)


def setup_inputs(seed: int = 0) -> dict:
    keys = jax.random.split(jax.random.key(seed), 17)
    tokens = normal_values(keys[0], (BATCH, D), 0.5, 3.0, ((0, 64),))
    attn_gain = jnp.clip(1.0 + 0.18 * jax.random.normal(keys[1], (D,), jnp.float32), 0.1, 1.9)
    w_query = normal_values(keys[2], (D, HEADS * HEAD), D ** -0.5, 0.1875, ((1, 4),))
    w_key = normal_values(keys[3], (D, KV_HEADS * HEAD), D ** -0.5, 0.1875, ((1, 4),))
    w_value = normal_values(keys[4], (D, KV_HEADS * HEAD), D ** -0.5, 0.1875, ((1, 4),))
    attn_bias = jnp.clip(-7.5 + 4.5 * jax.random.uniform(keys[5], (HEADS,), jnp.float32) ** level_of(keys[5], (HEADS,), ((0, 4),), -0.2, 0.2), -7.5, -3.0)
    key_cache = normal_values(keys[6], (BATCH, KV_HEADS * HEAD, LEN), 1.0, 6.0, ((0, 64), (1, 4)))
    value_cache = normal_values(keys[7], (BATCH, KV_HEADS * HEAD, LEN), 1.0, 6.0, ((0, 64), (1, 4)))
    lengths = set_ends(jax.random.randint(keys[8], (BATCH,), LEN // 8, LEN + 1), jax.random.fold_in(keys[8], 1), LEN // 8, LEN).astype(jnp.int32)
    w_out = normal_values(keys[9], (HEADS * HEAD, D), (HEADS * HEAD // 16) ** -0.5, 0.75, ((0, 4),))
    ffn_gain = jnp.clip(1.0 + 0.18 * jax.random.normal(keys[10], (D,), jnp.float32), 0.1, 1.9)
    routes_keys = jax.random.split(jax.random.fold_in(keys[11], 1), BATCH // SEQS)
    routes_turns = jax.random.permutation(jax.random.fold_in(keys[11], 3), BATCH // SEQS)
    routes = jax.vmap(lambda own, number: routed_block(jax.random.fold_in(keys[11], 2), own, number, SEQS, EXPERTS, TOP, CAP, 1))(routes_keys, routes_turns).reshape((BATCH, TOP))
    route_weight = jnp.clip(0.2 + 0.8 * jax.random.uniform(keys[12], (BATCH, TOP), jnp.float32) ** level_of(keys[12], (BATCH, TOP), ((0, 64),), -0.2, 0.2), 0.2, 1.0)
    expert_gate = normal_values(keys[13], (EXPERTS, D, FF), D ** -0.5, 0.1875, ((0, 64), (2, 4)))
    expert_up = normal_values(keys[14], (EXPERTS, D, FF), D ** -0.5, 0.1875, ((0, 64), (2, 4)))
    expert_down = normal_values(keys[15], (EXPERTS, FF, D), FF ** -0.5, 0.09375, ((0, 64), (1, 4)))
    return {"tokens": tokens, "attn_gain": attn_gain, "w_query": w_query, "w_key": w_key, "w_value": w_value, "attn_bias": attn_bias, "key_cache": key_cache, "value_cache": value_cache, "lengths": lengths, "w_out": w_out, "ffn_gain": ffn_gain, "routes": routes, "route_weight": route_weight, "expert_gate": expert_gate, "expert_up": expert_up, "expert_down": expert_down}


norm_epsilon = 1e-06

def rms_scale(inputs, gains):
    widened = inputs.astype(jnp.float32)
    factor = lax.rsqrt(lax.optimization_barrier(jnp.mean(widened * widened, axis=-1, keepdims=True)) + norm_epsilon)
    return (widened * factor * gains).astype(jnp.bfloat16)

def dispatch_matrix(block_routes, experts, capacity):
    flat_routes = block_routes.reshape(-1).astype(jnp.int32)
    onehot = (flat_routes[:, None] == jnp.arange(experts, dtype=jnp.int32)[None, :]).astype(jnp.int32)
    before = (jnp.cumsum(onehot, axis=0) - onehot).astype(jnp.int32)
    slot_index = lax.optimization_barrier(jnp.sum(before * onehot, axis=1)).astype(jnp.int32)
    target = flat_routes * capacity + slot_index
    return jnp.arange(experts * capacity, dtype=jnp.int32)[:, None] == target[None, :]

def stick_read(queries, key_block, value_block, bias_grid, lengths):
    row_count, kv_count, group_size, head_size = queries.shape
    key_span = key_block.shape[2]
    key_heads = key_block.reshape(row_count, kv_count, head_size, key_span).astype(jnp.float32)
    value_heads = value_block.reshape(row_count, kv_count, head_size, key_span).astype(jnp.float32)
    scores = jnp.einsum('skgd,skdl->skgl', queries.astype(jnp.float32), key_heads) * head_size ** (-0.5)
    scores = scores + bias_grid[None, :, :, None]
    inside = (jnp.arange(key_span, dtype=jnp.int32)[None, :] < lengths[:, None])[:, None, None, :]
    log_fall = jnp.where(inside, jax.nn.log_sigmoid(-scores), 0.0)
    log_after = lax.cumsum(log_fall, axis=3, reverse=True) - log_fall
    weights = jnp.where(inside, jnp.exp(jax.nn.log_sigmoid(scores) + log_after), 0.0).astype(jnp.bfloat16)
    mixed_out = jnp.einsum('skgl,skdl->skgd', weights.astype(jnp.float32), value_heads)
    return mixed_out.astype(jnp.bfloat16).reshape(row_count, -1)

def expert_rows(operands):
    row_block, gate_matrix, up_matrix, down_matrix = operands
    gate_act = jnp.dot(row_block, gate_matrix, preferred_element_type=jnp.float32)
    lifted = jnp.dot(row_block, up_matrix, preferred_element_type=jnp.float32)
    hidden = (jax.nn.silu(gate_act) * lifted).astype(jnp.bfloat16)
    pieces = jnp.einsum('rtf,tfd->rtd', hidden.reshape(hidden.shape[0], N_TP, -1).astype(jnp.float32), down_matrix.reshape(N_TP, -1, down_matrix.shape[1]).astype(jnp.float32))
    rounded = lax.optimization_barrier(pieces.astype(jnp.bfloat16))
    return lax.optimization_barrier(jnp.sum(rounded.astype(jnp.float32), axis=1)).astype(jnp.bfloat16)

def block_plan(block_routes):
    return dispatch_matrix(block_routes, EXPERTS, CAP)

def reference(tokens, attn_gain, w_query, w_key, w_value, attn_bias, key_cache, value_cache, lengths, w_out, ffn_gain, routes, route_weight, expert_gate, expert_up, expert_down):
    normed = rms_scale(tokens, attn_gain)
    queries = jnp.dot(normed, w_query, preferred_element_type=jnp.float32).astype(jnp.bfloat16)
    new_keys = jnp.dot(normed, w_key, preferred_element_type=jnp.float32).astype(jnp.bfloat16)
    new_values = jnp.dot(normed, w_value, preferred_element_type=jnp.float32).astype(jnp.bfloat16)
    group_size = HEADS // KV_HEADS
    grouped = queries.reshape(N_EP, SEQS, KV_HEADS, group_size, HEAD)
    bias_grid = attn_bias.reshape(KV_HEADS, group_size)

    def per_block(block_args):
        return stick_read(block_args[0], block_args[1], block_args[2], bias_grid, block_args[3])
    attended = lax.map(per_block, (grouped, key_cache.reshape(N_EP, SEQS, KV_HEADS * HEAD, LEN), value_cache.reshape(N_EP, SEQS, KV_HEADS * HEAD, LEN), lengths.reshape(N_EP, SEQS)))
    attended = attended.reshape(BATCH, HEADS * HEAD)
    parts = jnp.einsum('btf,tfd->btd', attended.reshape(BATCH, N_TP, -1).astype(jnp.float32), w_out.reshape(N_TP, -1, D).astype(jnp.float32))
    rounded = lax.optimization_barrier(parts.astype(jnp.bfloat16))
    attn_total = lax.optimization_barrier(jnp.sum(rounded.astype(jnp.float32), axis=1))
    residual = (tokens.astype(jnp.float32) + attn_total).astype(jnp.bfloat16)
    normed_two = rms_scale(residual, ffn_gain)
    plans = jax.vmap(block_plan)(routes.reshape(N_EP, SEQS, TOP)).astype(jnp.float32)
    repeated = jnp.repeat(normed_two.reshape(N_EP, SEQS, 1, D), TOP, axis=2).reshape(N_EP, SEQS * TOP, D)
    sent = jnp.einsum('per,prd->ped', plans, repeated.astype(jnp.float32)).astype(jnp.bfloat16)
    received = sent.reshape(N_EP, EXPERTS, CAP, D).transpose(1, 0, 2, 3).reshape(EXPERTS, N_EP * CAP, D)
    outputs = lax.map(expert_rows, (received, expert_gate, expert_up, expert_down))
    back = outputs.reshape(EXPERTS, N_EP, CAP, D).transpose(1, 0, 2, 3).reshape(N_EP, EXPERTS * CAP, D)
    picked = jnp.einsum('per,ped->prd', plans, back.astype(jnp.float32)).reshape(BATCH, TOP, D)
    moe_sum = lax.optimization_barrier(jnp.sum(picked * route_weight[:, :, None], axis=1))
    mixed = (residual.astype(jnp.float32) + moe_sum).astype(jnp.bfloat16)
    return (mixed, new_keys, new_values)
```

```python
import jax
import jax.numpy as jnp
from jax import lax
from jax.experimental import pallas as pl
from jax.experimental.pallas import tpu as pltpu
from jax.sharding import PartitionSpec as P

MESH = pl.DeviceIdType.MESH
HEAD = 64
EPS = 1e-06
F32 = jnp.float32
BF16 = jnp.bfloat16


def rms(x, gain):
    factor = lax.rsqrt(jnp.mean(x * x, axis=-1, keepdims=True) + EPS)
    return (x * factor * gain).astype(BF16)


def iota(shape, dim):
    return lax.broadcasted_iota(jnp.int32, shape, dim)


def kernel(
    n_ep, n_tp,
    tok_h, again_h, wq_h, wk_h, wv_h, bias_h, key_h, val_h, len_h, wo_h, fgain_h, routes_h, rw_h, gate_h, up_h, down_h,
    mixed_o, nk_o, nv_o,
    tok, again, wq, wk, wv, bias, key, val, lens, wo, fgain, routes, rw, gate, up, down,
    tri, scores, part, part_in, disp, disp_in, back, back_in, fin, fin_in, wide, rows, hidden,
    in_sem, send_sem, recv_sem,
):
    ep, tp = lax.axis_index("ep"), lax.axis_index("tp")
    seqs, width = tok.shape
    groups = seqs // 8

    def load(n, src, dst):
        copy = pltpu.make_async_copy(src, dst, in_sem.at[n])
        copy.start()
        return copy

    c_tok = load(0, tok_h, tok)
    c_again = load(1, again_h, again)
    c_wq = load(2, wq_h, wq)
    c_bias = load(3, bias_h, bias)
    c_len = load(4, len_h, lens)
    c_key = [load(5 + g, key_h.at[pl.ds(8 * g, 8)], key.at[pl.ds(8 * g, 8)]) for g in range(groups)]
    c_val = [load(8 + g, val_h.at[pl.ds(8 * g, 8)], val.at[pl.ds(8 * g, 8)]) for g in range(groups)]
    c_wo = load(11, wo_h, wo)
    c_fgain = load(12, fgain_h, fgain)
    c_routes = load(13, routes_h, routes)
    c_rw = load(14, rw_h, rw)
    c_wk = load(15, wk_h, wk)
    c_wv = load(16, wv_h, wv)

    barrier = pltpu.get_barrier_semaphore()

    def greet_ep(i, carry):
        pl.semaphore_signal(barrier, inc=1, device_id=(lax.rem(ep + i, n_ep), tp), device_id_type=MESH)
        return carry

    def greet_tp(i, carry):
        pl.semaphore_signal(barrier, inc=1, device_id=(ep, lax.rem(tp + i, n_tp)), device_id_type=MESH)
        return carry

    lax.fori_loop(1, n_ep, greet_ep, 0)
    lax.fori_loop(1, n_tp, greet_tp, 0)

    tri[...] = jnp.where(iota((512, 256), 0) >= iota((512, 256), 1), 1.0, 0.0).astype(BF16)

    lane, sub = iota((8, 128), 1), iota((8, 128), 0)
    low = lane < 64
    own = [sub == 2 * j + jnp.where(low, 0, 1) for j in range(4)]

    c_tok.wait()
    c_again.wait()
    tokens = tok[...].astype(F32)
    normed = rms(tokens, again[...])
    c_wq.wait()
    queries = jnp.dot(normed, wq[...], preferred_element_type=F32).astype(BF16).astype(F32)

    c_bias.wait()
    c_len.wait()
    c_gate = load(17, gate_h.at[0], gate)
    c_up = load(18, up_h.at[0], up)
    c_down = load(19, down_h.at[0], down)

    for g in range(groups):
        blocks = []
        for h in range(4):
            half = queries[8 * g : 8 * g + 8, 128 * (h // 2) : 128 * (h // 2) + 128]
            turned = pltpu.roll(half, 64, 1)
            both = jnp.where(low, half, turned) if h % 2 == 0 else jnp.where(low, turned, half)
            blocks.append(jnp.concatenate([jnp.where(own[j], both, 0.0) for j in range(4)], axis=1))
        spread = jnp.concatenate(blocks, axis=0).astype(BF16)
        c_key[g].wait()
        raw = jnp.dot(spread, key[pl.ds(8 * g, 8)].reshape(512, 1024), preferred_element_type=F32)
        for h in range(4):
            scores[pl.ds(32 * g + 8 * h, 8), :] = raw[8 * h : 8 * h + 8] * HEAD**-0.5 + bias[h]

    position = iota((32, 1024), 1)
    attended = []
    for g in range(groups):
        s = scores[pl.ds(32 * g, 32), :]
        length = jnp.zeros((8, 128), jnp.int32)
        for r in range(8):
            length = jnp.where(sub == r, lens[8 * g + r], length)
        length = jnp.concatenate([length] * 8, axis=1)
        length = jnp.concatenate([length] * 4, axis=0)
        inside = position < length
        fall = jnp.where(inside, -(jnp.maximum(s, 0.0) + jnp.log(1.0 + jnp.exp(-jnp.abs(s)))), 0.0)
        pieces = [fall[:, 256 * b : 256 * b + 256] for b in range(4)]
        later = [None] * 4
        later[3] = jnp.zeros_like(pieces[3])
        for b in (2, 1, 0):
            later[b] = later[b + 1] + pieces[b + 1]
        stacked = jnp.concatenate([jnp.concatenate([pieces[b], later[b]], axis=1) for b in range(4)], axis=0)
        high = stacked.astype(BF16)
        rest = (stacked - high.astype(F32)).astype(BF16)
        total = jnp.dot(high, tri[...], preferred_element_type=F32) + jnp.dot(rest, tri[...], preferred_element_type=F32)
        total = jnp.concatenate([total[32 * b : 32 * b + 32] for b in range(4)], axis=1)
        weights = jnp.where(inside, jnp.exp(s + total), 0.0).astype(BF16)
        c_val[g].wait()
        mixed = lax.dot_general(
            weights, val[pl.ds(8 * g, 8)].reshape(512, 1024), (((1,), (1,)), ((), ())), preferred_element_type=F32
        )
        heads = []
        for h in range(4):
            m = [jnp.where(own[j], mixed[8 * h : 8 * h + 8, 128 * j : 128 * j + 128], 0.0) for j in range(4)]
            m = (m[0] + m[1]) + (m[2] + m[3])
            heads.append(m + pltpu.roll(m, 64, 1))
        attended.append(jnp.concatenate([jnp.where(low, heads[0], heads[1]), jnp.where(low, heads[2], heads[3])], axis=1))
    attended = jnp.concatenate(attended, axis=0).astype(BF16)
    c_wo.wait()
    part[...] = jnp.dot(attended, wo[...], preferred_element_type=F32).astype(BF16)

    pl.semaphore_wait(barrier, n_ep + n_tp - 2)

    def to_tp(src, dst, n):
        def send(i, carry):
            pltpu.make_async_remote_copy(
                src_ref=src, dst_ref=dst.at[tp], send_sem=send_sem.at[n], recv_sem=recv_sem.at[n],
                device_id=(ep, lax.rem(tp + i, n_tp)), device_id_type=MESH,
            ).start()
            return carry

        lax.fori_loop(1, n_tp, send, 0)

    def to_ep(src, dst, n):
        def send(i, carry):
            p = lax.rem(ep + i, n_ep)
            pltpu.make_async_remote_copy(
                src_ref=src.at[p], dst_ref=dst.at[ep], send_sem=send_sem.at[n], recv_sem=recv_sem.at[n],
                device_id=(p, tp), device_id_type=MESH,
            ).start()
            return carry

        lax.fori_loop(1, n_ep, send, 0)

    def arrived(dst, n, count, sems):
        some = dst.at[pl.ds(0, count)]
        pltpu.make_async_copy(some, some, sems.at[n]).wait()

    to_tp(part, part_in, 0)
    part_in[tp] = part[...]

    c_routes.wait()
    c_rw.wait()
    c_fgain.wait()
    lane24 = iota((seqs, 128), 1)
    expert = lane24 - jnp.where(lane24 >= n_ep, n_ep, 0)
    slot = jnp.where(lane24 >= n_ep, 1.0, 0.0)
    first = jnp.where(routes[:, 0:1] == expert, 1.0, 0.0)
    second = jnp.where(routes[:, 1:2] == expert, 1.0, 0.0)
    chosen = first + second
    below = jnp.where(iota((seqs, seqs), 0) > iota((seqs, seqs), 1), 1.0, 0.0)
    before = jnp.dot(below.astype(BF16), chosen.astype(BF16), preferred_element_type=F32)
    here = jnp.where(before == slot, 1.0, 0.0)
    plan = jnp.transpose(chosen * here).astype(BF16)
    gather = (first * rw[:, 0:1] + second * rw[:, 1:2]) * here
    gather_high = gather.astype(BF16)
    gather_rest = (gather - gather_high.astype(F32)).astype(BF16)
    c_wk.wait()
    nk_o[...] = jnp.dot(normed, wk[...], preferred_element_type=F32).astype(BF16)
    c_wv.wait()
    nv_o[...] = jnp.dot(normed, wv[...], preferred_element_type=F32).astype(BF16)

    arrived(part_in, 0, n_tp - 1, recv_sem)
    summed = part_in[0].astype(F32)
    for t in range(1, n_tp):
        summed = summed + part_in[t].astype(F32)
    residual = (tokens + summed).astype(BF16).astype(F32)
    normed_two = rms(residual, fgain[...])

    def store_rows(j, both):
        for s in range(2):
            wide[pl.ds(8 * s + j, n_ep, stride=16), :] = both[n_ep * s : n_ep * (s + 1)]

    def read_rows(j):
        return jnp.concatenate([wide[pl.ds(8 * s + j, n_ep, stride=16), :] for s in range(2)], axis=0)

    for j in range(8):
        store_rows(j, jnp.dot(plan, normed_two[:, 128 * j : 128 * j + 128], preferred_element_type=F32))
    disp[...] = wide[...].astype(BF16).reshape(n_ep, 16, 128)
    to_ep(disp, disp_in, 1)
    disp_in[ep] = disp[ep]

    c_gate.wait()
    c_up.wait()
    c_down.wait()
    arrived(disp_in, 1, n_ep - 1, recv_sem)
    wide[...] = disp_in[...].astype(F32).reshape(n_ep * 16, 128)
    for j in range(8):
        rows[:, 128 * j : 128 * j + 128] = read_rows(j).astype(BF16)

    units = gate.shape[1]
    for c in range(0, units, 256):
        size = min(256, units - c)
        a = jnp.dot(rows[...], gate[:, c : c + size], preferred_element_type=F32)
        b = jnp.dot(rows[...], up[:, c : c + size], preferred_element_type=F32)
        hidden[:, c : c + size] = (a / (1.0 + jnp.exp(-a)) * b).astype(BF16)
    for c in range(0, width, 256):
        out = jnp.dot(hidden[...], down[:, c : c + 256], preferred_element_type=F32)
        for i in range(2):
            store_rows(c // 128 + i, out[:, 128 * i : 128 * i + 128])
    back[...] = wide[...].astype(BF16).reshape(n_ep, 16, 128)
    to_ep(back, back_in, 2)
    back_in[ep] = back[ep]

    arrived(back_in, 2, n_ep - 1, recv_sem)
    wide[...] = back_in[...].astype(F32).reshape(n_ep * 16, 128)
    for j in range(8):
        rows[:, 128 * j : 128 * j + 128] = read_rows(j).astype(BF16)
    fin[...] = (
        jnp.dot(gather_high, rows[...], preferred_element_type=F32)
        + jnp.dot(gather_rest, rows[...], preferred_element_type=F32)
    ).astype(BF16)
    to_tp(fin, fin_in, 3)
    fin_in[tp] = fin[...]
    arrived(part_in, 0, n_tp - 1, send_sem)
    arrived(disp_in, 1, n_ep - 1, send_sem)
    arrived(back_in, 2, n_ep - 1, send_sem)
    arrived(fin_in, 3, n_tp - 1, recv_sem)
    summed = fin_in[0].astype(F32)
    for t in range(1, n_tp):
        summed = summed + fin_in[t].astype(F32)
    mixed_o[...] = (residual + summed).astype(BF16)
    arrived(fin_in, 3, n_tp - 1, send_sem)


def solution(mesh):
    n_ep, n_tp = mesh.shape["ep"], mesh.shape["tp"]

    def body(*args):
        (tokens, attn_gain, w_query, w_key, w_value, attn_bias, key_cache, value_cache, lengths, w_out,
         ffn_gain, routes, route_weight, expert_gate, expert_up, expert_down) = args
        seqs, width = tokens.shape
        units = expert_gate.shape[2]
        operands = (
            tokens, attn_gain.reshape(1, width), w_query, w_key, w_value, attn_bias, key_cache, value_cache, lengths,
            w_out, ffn_gain.reshape(1, width), routes, route_weight, expert_gate, expert_up, expert_down,
        )
        vmem, smem = pltpu.VMEM, pltpu.SMEM

        def run(*refs):
            kernel(n_ep, n_tp, *refs)

        return pl.pallas_call(
            run,
            name="layer",
            out_shape=(
                jax.ShapeDtypeStruct(tokens.shape, BF16),
                jax.ShapeDtypeStruct((seqs, w_key.shape[1]), BF16),
                jax.ShapeDtypeStruct((seqs, w_value.shape[1]), BF16),
            ),
            in_specs=[pl.BlockSpec(memory_space=pltpu.HBM)] * len(operands),
            out_specs=(pl.BlockSpec(memory_space=vmem),) * 3,
            scratch_shapes=[
                vmem(tokens.shape, BF16), vmem((1, width), F32), vmem(w_query.shape, BF16), vmem(w_key.shape, BF16),
                vmem(w_value.shape, BF16), smem(attn_bias.shape, F32), vmem(key_cache.shape, BF16),
                vmem(value_cache.shape, BF16), smem(lengths.shape, jnp.int32), vmem(w_out.shape, BF16),
                vmem((1, width), F32), vmem(routes.shape, jnp.int32), vmem(route_weight.shape, F32),
                vmem(expert_gate.shape[1:], BF16), vmem(expert_up.shape[1:], BF16), vmem(expert_down.shape[1:], BF16),
                vmem((512, 256), BF16), vmem((4 * seqs, 1024), F32), vmem(tokens.shape, BF16),
                vmem((n_tp, seqs, width), BF16), vmem((n_ep, 16, 128), BF16), vmem((n_ep, 16, 128), BF16),
                vmem((n_ep, 16, 128), BF16), vmem((n_ep, 16, 128), BF16), vmem(tokens.shape, BF16),
                vmem((n_tp, seqs, width), BF16), vmem((n_ep * 16, 128), F32), vmem((2 * n_ep, width), BF16),
                vmem((2 * n_ep, units), BF16),
                pltpu.SemaphoreType.DMA((20,)), pltpu.SemaphoreType.DMA((4,)), pltpu.SemaphoreType.DMA((4,)),
            ],
            compiler_params=pltpu.CompilerParams(
                collective_id=0, has_side_effects=True, vmem_limit_bytes=48 * 1024 * 1024
            ),
        )(*operands)

    return jax.shard_map(
        body,
        mesh=mesh,
        in_specs=(
            P("ep", None), P(), P(None, "tp"), P(None, "tp"), P(None, "tp"), P("tp"), P("ep", "tp", None),
            P("ep", "tp", None), P("ep"), P("tp", None), P(), P("ep", None), P("ep", None), P("ep", None, "tp"),
            P("ep", None, "tp"), P("ep", "tp", None),
        ),
        out_specs=(P("ep", None), P("ep", "tp"), P("ep", "tp")),
        check_vma=False,
    )
```

```python
import random

import jax
import jax.numpy as jnp
from jax import lax
from jax.experimental import pallas as pl
from jax.experimental.pallas import tpu as pltpu
from jax.sharding import PartitionSpec as P

MESH = pl.DeviceIdType.MESH
HEAD = 64
EPS = 1e-06
Z, Y, X = 8, 4, 2
F32 = jnp.float32
BF16 = jnp.bfloat16


def rms(x, gain):
    factor = lax.rsqrt(jnp.mean(x * x, axis=-1, keepdims=True) + EPS)
    return (x * factor * gain).astype(BF16)


def iota(shape, dim):
    return lax.broadcasted_iota(jnp.int32, shape, dim)


def far_first():
    offsets = [(z, y, x) for z in range(Z) for y in range(Y) for x in range(X)][1:]
    random.Random(0).shuffle(offsets)
    return sorted(offsets, key=lambda o: -(min(o[0], Z - o[0]) + min(o[1], Y - o[1]) + 2 * o[2]))


def kernel(
    n_ep, n_tp,
    tok_h, again_h, wq_h, wk_h, wv_h, bias_h, key_h, val_h, len_h, wo_h, fgain_h, routes_h, rw_h, gate_h, up_h, down_h,
    mixed_o, nk_o, nv_o,
    tok, again, wq, wk, wv, bias, key, val, lens, wo, fgain, routes, rw, gate, up, down,
    tri, scores, part, part_in, disp, disp_in, back, back_in, fin, fin_in, wide, rows, hidden,
    in_sem, send_sem, recv_sem,
):
    ep, tp = lax.axis_index("ep"), lax.axis_index("tp")
    z, y, x = ep // (Y * X), lax.rem(ep // X, Y), lax.rem(ep, X)
    seqs, width = tok.shape
    groups = seqs // 8

    def load(n, src, dst):
        copy = pltpu.make_async_copy(src, dst, in_sem.at[n])
        copy.start()
        return copy

    c_tok = load(0, tok_h, tok)
    c_again = load(1, again_h, again)
    c_wq = load(2, wq_h, wq)
    c_bias = load(3, bias_h, bias)
    c_len = load(4, len_h, lens)
    c_key = [load(5 + g, key_h.at[pl.ds(8 * g, 8)], key.at[pl.ds(8 * g, 8)]) for g in range(groups)]
    c_val = [load(8 + g, val_h.at[pl.ds(8 * g, 8)], val.at[pl.ds(8 * g, 8)]) for g in range(groups)]
    c_wo = load(11, wo_h, wo)
    c_fgain = load(12, fgain_h, fgain)
    c_routes = load(13, routes_h, routes)
    c_rw = load(14, rw_h, rw)
    c_wk = load(15, wk_h, wk)
    c_wv = load(16, wv_h, wv)

    barrier = pltpu.get_barrier_semaphore()

    def greet_ep(i, carry):
        pl.semaphore_signal(barrier, inc=1, device_id=(lax.rem(ep + i, n_ep), tp), device_id_type=MESH)
        return carry

    def greet_tp(i, carry):
        pl.semaphore_signal(barrier, inc=1, device_id=(ep, lax.rem(tp + i, n_tp)), device_id_type=MESH)
        return carry

    lax.fori_loop(1, n_ep, greet_ep, 0)
    lax.fori_loop(1, n_tp, greet_tp, 0)

    tri[...] = jnp.where(iota((512, 256), 0) >= iota((512, 256), 1), 1.0, 0.0).astype(BF16)

    lane, sub = iota((8, 128), 1), iota((8, 128), 0)
    low = lane < 64
    own = [sub == 2 * j + jnp.where(low, 0, 1) for j in range(4)]

    c_tok.wait()
    c_again.wait()
    tokens = tok[...].astype(F32)
    normed = rms(tokens, again[...])
    c_wq.wait()
    queries = jnp.dot(normed, wq[...], preferred_element_type=F32).astype(BF16).astype(F32)

    c_bias.wait()
    c_len.wait()
    c_gate = load(17, gate_h.at[0], gate)
    c_up = load(18, up_h.at[0], up)
    c_down = load(19, down_h.at[0], down)

    for g in range(groups):
        blocks = []
        for h in range(4):
            half = queries[8 * g : 8 * g + 8, 128 * (h // 2) : 128 * (h // 2) + 128]
            turned = pltpu.roll(half, 64, 1)
            both = jnp.where(low, half, turned) if h % 2 == 0 else jnp.where(low, turned, half)
            blocks.append(jnp.concatenate([jnp.where(own[j], both, 0.0) for j in range(4)], axis=1))
        spread = jnp.concatenate(blocks, axis=0).astype(BF16)
        c_key[g].wait()
        raw = jnp.dot(spread, key[pl.ds(8 * g, 8)].reshape(512, 1024), preferred_element_type=F32)
        for h in range(4):
            scores[pl.ds(32 * g + 8 * h, 8), :] = raw[8 * h : 8 * h + 8] * HEAD**-0.5 + bias[h]

    position = iota((32, 1024), 1)
    attended = []
    for g in range(groups):
        s = scores[pl.ds(32 * g, 32), :]
        length = jnp.zeros((8, 128), jnp.int32)
        for r in range(8):
            length = jnp.where(sub == r, lens[8 * g + r], length)
        length = jnp.concatenate([length] * 8, axis=1)
        length = jnp.concatenate([length] * 4, axis=0)
        inside = position < length
        fall = jnp.where(inside, -(jnp.maximum(s, 0.0) + jnp.log(1.0 + jnp.exp(-jnp.abs(s)))), 0.0)
        pieces = [fall[:, 256 * b : 256 * b + 256] for b in range(4)]
        later = [None] * 4
        later[3] = jnp.zeros_like(pieces[3])
        for b in (2, 1, 0):
            later[b] = later[b + 1] + pieces[b + 1]
        stacked = jnp.concatenate([jnp.concatenate([pieces[b], later[b]], axis=1) for b in range(4)], axis=0)
        high = stacked.astype(BF16)
        rest = (stacked - high.astype(F32)).astype(BF16)
        total = jnp.dot(high, tri[...], preferred_element_type=F32) + jnp.dot(rest, tri[...], preferred_element_type=F32)
        total = jnp.concatenate([total[32 * b : 32 * b + 32] for b in range(4)], axis=1)
        weights = jnp.where(inside, jnp.exp(s + total), 0.0).astype(BF16)
        c_val[g].wait()
        mixed = lax.dot_general(
            weights, val[pl.ds(8 * g, 8)].reshape(512, 1024), (((1,), (1,)), ((), ())), preferred_element_type=F32
        )
        heads = []
        for h in range(4):
            m = [jnp.where(own[j], mixed[8 * h : 8 * h + 8, 128 * j : 128 * j + 128], 0.0) for j in range(4)]
            m = (m[0] + m[1]) + (m[2] + m[3])
            heads.append(m + pltpu.roll(m, 64, 1))
        attended.append(jnp.concatenate([jnp.where(low, heads[0], heads[1]), jnp.where(low, heads[2], heads[3])], axis=1))
    attended = jnp.concatenate(attended, axis=0).astype(BF16)
    c_wo.wait()
    part[...] = jnp.dot(attended, wo[...], preferred_element_type=F32).astype(BF16)

    pl.semaphore_wait(barrier, n_ep + n_tp - 2)

    def to_tp(src, dst, n):
        def send(i, carry):
            pltpu.make_async_remote_copy(
                src_ref=src, dst_ref=dst.at[tp], send_sem=send_sem.at[n], recv_sem=recv_sem.at[n],
                device_id=(ep, lax.rem(tp + i, n_tp)), device_id_type=MESH,
            ).start()
            return carry

        lax.fori_loop(1, n_tp, send, 0)

    def to_ep(src, dst, n):
        for dz, dy, dx in far_first():
            p = (lax.rem(z + dz, Z) * Y + lax.rem(y + dy, Y)) * X + lax.rem(x + dx, X)
            pltpu.make_async_remote_copy(
                src_ref=src.at[p], dst_ref=dst.at[ep], send_sem=send_sem.at[n], recv_sem=recv_sem.at[n],
                device_id=(p, tp), device_id_type=MESH,
            ).start()

    def arrived(dst, n, count, sems):
        some = dst.at[pl.ds(0, count)]
        pltpu.make_async_copy(some, some, sems.at[n]).wait()

    to_tp(part, part_in, 0)
    part_in[tp] = part[...]

    c_routes.wait()
    c_rw.wait()
    c_fgain.wait()
    place = iota((2 * n_ep, seqs), 0)
    expert = place - jnp.where(place >= n_ep, n_ep, 0)
    slot = jnp.where(place >= n_ep, 1.0, 0.0)
    first = jnp.where(routes[0:1, :] == expert, 1.0, 0.0)
    second = jnp.where(routes[1:2, :] == expert, 1.0, 0.0)
    chosen = first + second
    above = jnp.where(iota((seqs, seqs), 0) < iota((seqs, seqs), 1), 1.0, 0.0)
    before = jnp.dot(chosen.astype(BF16), above.astype(BF16), preferred_element_type=F32)
    here = jnp.where(before == slot, 1.0, 0.0)
    plan = (chosen * here).astype(BF16)
    gather = jnp.transpose((first * rw[0:1, :] + second * rw[1:2, :]) * here)
    gather_high = gather.astype(BF16)
    gather_rest = (gather - gather_high.astype(F32)).astype(BF16)
    turned = (((1,), (1,)), ((), ()))
    c_wk.wait()
    nk_o[...] = lax.dot_general(normed, wk[...], turned, preferred_element_type=F32).astype(BF16)
    c_wv.wait()
    nv_o[...] = lax.dot_general(normed, wv[...], turned, preferred_element_type=F32).astype(BF16)

    arrived(part_in, 0, n_tp - 1, recv_sem)
    summed = part_in[0].astype(F32)
    for t in range(1, n_tp):
        summed = summed + part_in[t].astype(F32)
    residual = (tokens + summed).astype(BF16).astype(F32)
    normed_two = rms(residual, fgain[...])

    def store_rows(j, both):
        for s in range(2):
            wide[pl.ds(8 * s + j, n_ep, stride=16), :] = both[n_ep * s : n_ep * (s + 1)]

    def read_rows(j):
        return jnp.concatenate([wide[pl.ds(8 * s + j, n_ep, stride=16), :] for s in range(2)], axis=0)

    for j in range(8):
        store_rows(j, jnp.dot(plan, normed_two[:, 128 * j : 128 * j + 128], preferred_element_type=F32))
    disp[...] = wide[...].astype(BF16).reshape(n_ep, 16, 128)
    to_ep(disp, disp_in, 1)
    disp_in[ep] = disp[ep]

    c_gate.wait()
    c_up.wait()
    c_down.wait()
    arrived(disp_in, 1, n_ep - 1, recv_sem)
    wide[...] = disp_in[...].astype(F32).reshape(n_ep * 16, 128)
    for j in range(8):
        rows[:, 128 * j : 128 * j + 128] = read_rows(j).astype(BF16)

    units = gate.shape[1]
    for c in range(0, units, 256):
        size = min(256, units - c)
        a = jnp.dot(rows[...], gate[:, c : c + size], preferred_element_type=F32)
        b = jnp.dot(rows[...], up[:, c : c + size], preferred_element_type=F32)
        hidden[:, c : c + size] = (a / (1.0 + jnp.exp(-a)) * b).astype(BF16)
    for c in range(0, width, 256):
        out = jnp.dot(hidden[...], down[:, c : c + 256], preferred_element_type=F32)
        for i in range(2):
            store_rows(c // 128 + i, out[:, 128 * i : 128 * i + 128])
    back[...] = wide[...].astype(BF16).reshape(n_ep, 16, 128)
    to_ep(back, back_in, 2)
    back_in[ep] = back[ep]

    arrived(back_in, 2, n_ep - 1, recv_sem)
    wide[...] = back_in[...].astype(F32).reshape(n_ep * 16, 128)
    for j in range(8):
        rows[:, 128 * j : 128 * j + 128] = read_rows(j).astype(BF16)
    fin[...] = (
        jnp.dot(gather_high, rows[...], preferred_element_type=F32)
        + jnp.dot(gather_rest, rows[...], preferred_element_type=F32)
    ).astype(BF16)
    to_tp(fin, fin_in, 3)
    fin_in[tp] = fin[...]
    arrived(part_in, 0, n_tp - 1, send_sem)
    arrived(disp_in, 1, n_ep - 1, send_sem)
    arrived(back_in, 2, n_ep - 1, send_sem)
    arrived(fin_in, 3, n_tp - 1, recv_sem)
    summed = fin_in[0].astype(F32)
    for t in range(1, n_tp):
        summed = summed + fin_in[t].astype(F32)
    mixed_o[...] = (residual + summed).astype(BF16)
    arrived(fin_in, 3, n_tp - 1, send_sem)


def write_out(*refs):
    ins, outs, sems = refs[:3], refs[3:6], refs[6]
    copies = [pltpu.make_async_copy(ins[i], outs[i], sems.at[i]) for i in range(3)]
    for copy in copies:
        copy.start()
    for copy in copies:
        copy.wait()


def solution(mesh):
    n_ep, n_tp = mesh.shape["ep"], mesh.shape["tp"]

    def body(*args):
        (tokens, attn_gain, w_query, w_key, w_value, attn_bias, key_cache, value_cache, lengths, w_out,
         ffn_gain, routes, route_weight, expert_gate, expert_up, expert_down) = args
        seqs, width = tokens.shape
        units = expert_gate.shape[2]
        operands = (
            tokens, attn_gain.reshape(1, width), w_query, w_key.T, w_value.T, attn_bias, key_cache, value_cache, lengths,
            w_out, ffn_gain.reshape(1, width), routes.T, route_weight.T, expert_gate, expert_up, expert_down,
        )
        vmem, smem = pltpu.VMEM, pltpu.SMEM

        def run(*refs):
            kernel(n_ep, n_tp, *refs)

        results = pl.pallas_call(
            run,
            name="layer",
            out_shape=(
                jax.ShapeDtypeStruct(tokens.shape, BF16),
                jax.ShapeDtypeStruct((seqs, w_key.shape[1]), BF16),
                jax.ShapeDtypeStruct((seqs, w_value.shape[1]), BF16),
            ),
            in_specs=[pl.BlockSpec(memory_space=pltpu.HBM)] * len(operands),
            out_specs=(pl.BlockSpec(memory_space=vmem),) * 3,
            scratch_shapes=[
                vmem(tokens.shape, BF16), vmem((1, width), F32), vmem(w_query.shape, BF16), vmem(w_key.shape[::-1], BF16),
                vmem(w_value.shape[::-1], BF16), smem(attn_bias.shape, F32), vmem(key_cache.shape, BF16),
                vmem(value_cache.shape, BF16), smem(lengths.shape, jnp.int32), vmem(w_out.shape, BF16),
                vmem((1, width), F32), vmem(routes.shape[::-1], jnp.int32), vmem(route_weight.shape[::-1], F32),
                vmem(expert_gate.shape[1:], BF16), vmem(expert_up.shape[1:], BF16), vmem(expert_down.shape[1:], BF16),
                vmem((512, 256), BF16), vmem((4 * seqs, 1024), F32), vmem(tokens.shape, BF16),
                vmem((n_tp, seqs, width), BF16), vmem((n_ep, 16, 128), BF16), vmem((n_ep, 16, 128), BF16),
                vmem((n_ep, 16, 128), BF16), vmem((n_ep, 16, 128), BF16), vmem(tokens.shape, BF16),
                vmem((n_tp, seqs, width), BF16), vmem((n_ep * 16, 128), F32), vmem((2 * n_ep, width), BF16),
                vmem((2 * n_ep, units), BF16),
                pltpu.SemaphoreType.DMA((20,)), pltpu.SemaphoreType.DMA((4,)), pltpu.SemaphoreType.DMA((4,)),
            ],
            compiler_params=pltpu.CompilerParams(
                collective_id=0, has_side_effects=True, vmem_limit_bytes=48 * 1024 * 1024
            ),
        )(*[pltpu.with_memory_space_constraint(x, pltpu.HBM) for x in operands])

        return pl.pallas_call(
            write_out,
            name="write_out",
            out_shape=tuple(pltpu.HBM(r.shape, r.dtype) for r in results),
            in_specs=[pl.BlockSpec(memory_space=vmem)] * 3,
            out_specs=(pl.BlockSpec(memory_space=pltpu.HBM),) * 3,
            scratch_shapes=[pltpu.SemaphoreType.DMA((3,))],
            compiler_params=pltpu.CompilerParams(vmem_limit_bytes=1024 * 1024),
        )(*[pltpu.with_memory_space_constraint(r, vmem) for r in results])

    return jax.shard_map(
        body,
        mesh=mesh,
        in_specs=(
            P("ep", None), P(), P(None, "tp"), P(None, "tp"), P(None, "tp"), P("tp"), P("ep", "tp", None),
            P("ep", "tp", None), P("ep"), P("tp", None), P(), P("ep", None), P("ep", None), P("ep", None, "tp"),
            P("ep", None, "tp"), P("ep", "tp", None),
        ),
        out_specs=(P("ep", None), P("ep", "tp"), P("ep", "tp")),
        check_vma=False,
    )
```

```python
import random

import jax
import jax.numpy as jnp
from jax import lax
from jax.experimental import pallas as pl
from jax.experimental.pallas import tpu as pltpu
from jax.sharding import PartitionSpec as P

MESH = pl.DeviceIdType.MESH
HEAD = 64
EPS = 1e-06
PARTS, FAR, NEAR, PAIR_FAR, PAIR_NEAR, PAIR_BACK, BACK, LAST, RESIDUAL = range(9)
Z, Y, X = 8, 4, 2
F32 = jnp.float32
BF16 = jnp.bfloat16


def rms(x, gain):
    factor = lax.rsqrt(jnp.mean(x * x, axis=-1, keepdims=True) + EPS)
    return (x * factor * gain).astype(BF16)


def iota(shape, dim):
    return lax.broadcasted_iota(jnp.int32, shape, dim)


def far_first():
    offsets = [(z, y, x) for z in range(Z) for y in range(Y) for x in range(X)][1:]
    random.Random(0).shuffle(offsets)
    return sorted(offsets, key=lambda o: -(min(o[0], Z - o[0]) + min(o[1], Y - o[1]) + 2 * o[2]))


def kernel(
    n_ep, n_tp,
    tok_h, again_h, wq_h, wk_h, wv_h, bias_h, key_h, val_h, len_h, wo_h, fgain_h, routes_h, rw_h, gate_h, up_h, down_h,
    mixed_o, nk_o, nv_o,
    tok, again, wq, wk, wv, bias, key, val, lens, wo, fgain, routes, rw, gate, up, down,
    tri, scores, falls_ref, part, part_in, disp, disp_in, disp_other, back, back_in, pair_out, pair_in, fin, fin_in, res_mine, res_other,
    wide, plain, rows, hidden,
    in_sem, send_sem, recv_sem,
):
    ep, tp = lax.axis_index("ep"), lax.axis_index("tp")
    z, y, x = ep // (Y * X), lax.rem(ep // X, Y), lax.rem(ep, X)
    zs = [lax.rem(z + d, Z) * (Y * X) for d in range(Z)]
    ys = [lax.rem(y + d, Y) * X for d in range(Y)]
    xs = [lax.rem(x + d, X) for d in range(X)]
    order = far_first()
    targets = [(zs[dz] + ys[dy]) + xs[dx] for dz, dy, dx in order]
    sources = [(zs[-dz % Z] + ys[-dy % Y]) + xs[-dx % X] for dz, dy, dx in order]
    core = lax.rem(tp, 2)
    partner = tp + 1 - 2 * core
    half_width = tok.shape[1] // 2
    far = n_ep // 2
    seqs, width = tok.shape
    groups = seqs // 8

    def load(n, src, dst):
        copy = pltpu.make_async_copy(src, dst, in_sem.at[n])
        copy.start()
        return copy

    c_tok = load(0, tok_h, tok)
    c_again = load(1, again_h, again)
    c_wq = load(2, wq_h, wq)
    c_bias = load(3, bias_h, bias)
    c_len = load(4, len_h, lens)
    c_key = [load(5 + g, key_h.at[pl.ds(8 * g, 8)], key.at[pl.ds(8 * g, 8)]) for g in range(groups)]
    c_val = [load(8 + g, val_h.at[pl.ds(8 * g, 8)], val.at[pl.ds(8 * g, 8)]) for g in range(groups)]
    c_wo = load(11, wo_h, wo)
    c_fgain = load(12, fgain_h, fgain)
    c_routes = load(13, routes_h, routes)
    c_rw = load(14, rw_h, rw)
    c_wk = load(15, wk_h, wk)
    c_wv = load(16, wv_h, wv)

    barrier = pltpu.get_barrier_semaphore()
    for p in targets:
        pl.semaphore_signal(barrier, inc=1, device_id=(p, tp), device_id_type=MESH)
    for i in range(1, n_tp):
        pl.semaphore_signal(barrier, inc=1, device_id=(ep, lax.rem(tp + i, n_tp)), device_id_type=MESH)

    tri[...] = jnp.where(iota((512, 256), 0) >= iota((512, 256), 1), 1.0, 0.0).astype(BF16)

    lane, sub = iota((8, 128), 1), iota((8, 128), 0)
    low = lane < 64
    own = [sub == 2 * j + jnp.where(low, 0, 1) for j in range(4)]

    c_tok.wait()
    c_again.wait()
    tokens = tok[...].astype(F32)
    normed = rms(tokens, again[...])
    c_wq.wait()
    queries = jnp.dot(normed, wq[...], preferred_element_type=F32).astype(BF16).astype(F32) * HEAD**-0.5

    c_bias.wait()
    c_len.wait()
    c_gate = load(17, gate_h.at[0], gate)
    c_up = load(18, up_h.at[0], up)
    c_down = load(19, down_h.at[0], down)

    position = iota((32, 1024), 1)
    for g in range(groups):
        blocks = []
        for h in range(4):
            half = queries[8 * g : 8 * g + 8, 128 * (h // 2) : 128 * (h // 2) + 128]
            turned = pltpu.roll(half, 64, 1)
            both = jnp.where(low, half, turned) if h % 2 == 0 else jnp.where(low, turned, half)
            blocks.append(jnp.concatenate([jnp.where(own[j], both, 0.0) for j in range(4)], axis=1))
        spread = jnp.concatenate(blocks, axis=0).astype(BF16)
        c_key[g].wait()
        raw = jnp.dot(spread, key[pl.ds(8 * g, 8)].reshape(512, 1024), preferred_element_type=F32)
        s = jnp.concatenate([raw[8 * h : 8 * h + 8] + bias[h] for h in range(4)], axis=0)
        length = jnp.zeros((8, 128), jnp.int32)
        for r in range(8):
            length = jnp.where(sub == r, lens[8 * g + r], length)
        length = jnp.concatenate([length] * 8, axis=1)
        length = jnp.concatenate([length] * 4, axis=0)
        inside = position < length
        fall = jnp.where(inside, jnp.minimum(-s, 0.0) - jnp.log(1.0 + jnp.exp(-jnp.abs(s))), 0.0)
        scores[pl.ds(32 * g, 32), :] = jnp.where(inside, s, -jnp.inf)
        pieces = [fall[:, 256 * b : 256 * b + 256] for b in range(4)]
        later = [None] * 4
        later[3] = jnp.zeros_like(pieces[3])
        for b in (2, 1, 0):
            later[b] = later[b + 1] + pieces[b + 1]
        for b in range(4):
            stacked = jnp.concatenate([pieces[b], later[b]], axis=1)
            high = stacked.astype(BF16)
            at = 128 * g + 32 * b
            falls_ref[pl.ds(at, 32), :] = high
            falls_ref[pl.ds(128 * groups + at, 32), :] = (stacked - high.astype(F32)).astype(BF16)

    total = jnp.dot(falls_ref[pl.ds(0, 128 * groups), :], tri[...], preferred_element_type=F32) + jnp.dot(
        falls_ref[pl.ds(128 * groups, 128 * groups), :], tri[...], preferred_element_type=F32
    )
    weights = []
    for g in range(groups):
        here = jnp.concatenate([total[128 * g + 32 * b : 128 * g + 32 * b + 32] for b in range(4)], axis=1)
        weights.append(jnp.exp(scores[pl.ds(32 * g, 32), :] + here).astype(BF16))
    for g in range(groups):
        c_val[g].wait()
    attended = []
    for g in range(groups):
        mixed = lax.dot_general(
            weights[g], val[pl.ds(8 * g, 8)].reshape(512, 1024), (((1,), (1,)), ((), ())), preferred_element_type=F32
        )
        heads = []
        for h in range(4):
            m = [jnp.where(own[j], mixed[8 * h : 8 * h + 8, 128 * j : 128 * j + 128], 0.0) for j in range(4)]
            m = (m[0] + m[1]) + (m[2] + m[3])
            heads.append(m + pltpu.roll(m, 64, 1))
        attended.append(jnp.concatenate([jnp.where(low, heads[0], heads[1]), jnp.where(low, heads[2], heads[3])], axis=1))
    attended = jnp.concatenate(attended, axis=0).astype(BF16)
    c_wo.wait()
    part_out = jnp.dot(attended, wo[...], preferred_element_type=F32).astype(BF16)
    for h in range(2):
        part[h] = part_out[:, half_width * h : half_width * (h + 1)]

    pl.semaphore_wait(barrier, n_ep + n_tp - 2)

    def push(src, dst, n, device):
        pltpu.make_async_remote_copy(
            src_ref=src, dst_ref=dst, send_sem=send_sem.at[n], recv_sem=recv_sem.at[n],
            device_id=device, device_id_type=MESH,
        ).start()

    def landed(some, n, sems):
        pltpu.make_async_copy(some, some, sems.at[n]).wait()

    for i in range(1, n_tp):
        t = lax.rem(tp + i, n_tp)
        push(part.at[lax.rem(t, 2)], part_in.at[tp], PARTS, (ep, t))
    part_in[tp] = part[core]

    c_routes.wait()
    c_rw.wait()
    c_fgain.wait()
    place = iota((2 * n_ep, seqs), 0)
    expert = place - jnp.where(place >= n_ep, n_ep, 0)
    slot = jnp.where(place >= n_ep, 1.0, 0.0)
    first = jnp.where(routes[0:1, :] == expert, 1.0, 0.0)
    second = jnp.where(routes[1:2, :] == expert, 1.0, 0.0)
    chosen = first + second
    above = jnp.where(iota((seqs, seqs), 0) < iota((seqs, seqs), 1), 1.0, 0.0)
    before = jnp.dot(chosen.astype(BF16), above.astype(BF16), preferred_element_type=F32)
    here = jnp.where(before == slot, 1.0, 0.0)
    plan = (chosen * here).astype(BF16)
    gather = jnp.transpose((first * rw[0:1, :] + second * rw[1:2, :]) * here)
    gather_high = gather.astype(BF16)
    gather_rest = (gather - gather_high.astype(F32)).astype(BF16)
    turned = (((1,), (1,)), ((), ()))
    c_wk.wait()
    nk_o[...] = lax.dot_general(normed, wk[...], turned, preferred_element_type=F32).astype(BF16)
    c_wv.wait()
    nv_o[...] = lax.dot_general(normed, wv[...], turned, preferred_element_type=F32).astype(BF16)

    landed(part_in.at[pl.ds(0, n_tp - 1)], PARTS, recv_sem)
    summed = part_in[0].astype(F32)
    for t in range(1, n_tp):
        summed = summed + part_in[t].astype(F32)
    token_half = jnp.where(core == 0, tokens[:, :half_width], tokens[:, half_width:])
    residual = (token_half + summed).astype(BF16)

    def store_rows(j, both):
        for s in range(2):
            wide[pl.ds(4 * s + j, n_ep, stride=8), :] = both[n_ep * s : n_ep * (s + 1)]

    def read_rows(j):
        return jnp.concatenate([wide[pl.ds(4 * s + j, n_ep, stride=8), :] for s in range(2)], axis=0)

    for j in range(4):
        store_rows(j, jnp.dot(plan, residual[:, 128 * j : 128 * j + 128], preferred_element_type=F32))
    disp[...] = wide[...].astype(BF16).reshape(n_ep, 8, 128)
    for k, p in enumerate(targets):
        push(disp.at[p], disp_in.at[k], FAR if k < far else NEAR, (p, tp))
    disp_in[n_ep - 1] = disp[ep]
    res_mine[...] = residual
    push(res_mine, res_other, RESIDUAL, (ep, partner))

    far_slots, near_slots = pl.ds(0, far), pl.ds(far, far)
    landed(disp_in.at[pl.ds(far, far - 1)], NEAR, recv_sem)
    push(disp_in.at[near_slots], disp_other.at[near_slots], PAIR_NEAR, (ep, partner))
    c_gate.wait()
    c_up.wait()
    c_down.wait()
    landed(disp_in.at[far_slots], FAR, recv_sem)
    push(disp_in.at[far_slots], disp_other.at[far_slots], PAIR_FAR, (ep, partner))

    def columns(h, j, size):
        return pl.ds(pl.multiple_of(half_width * h + size * j, size), size)

    squares = jnp.zeros((2 * n_ep, 128), F32)
    for h, block in ((core, disp_in), (1 - core, disp_other)):
        if block is disp_other:
            landed(disp_other.at[near_slots], PAIR_NEAR, recv_sem)
            landed(disp_other.at[far_slots], PAIR_FAR, recv_sem)
        wide[...] = block[...].astype(F32).reshape(n_ep * 8, 128)
        for j in range(4):
            values = read_rows(j)
            squares = squares + values * values
            plain[:, columns(h, j, 128)] = values
    factor = lax.rsqrt(jnp.sum(squares, axis=-1, keepdims=True) / width + EPS)
    rows[...] = (plain[...] * factor * fgain[...]).astype(BF16)

    units = gate.shape[1]
    for c in range(0, units, 256):
        size = min(256, units - c)
        a = jnp.dot(rows[...], gate[:, c : c + size], preferred_element_type=F32)
        b = jnp.dot(rows[...], up[:, c : c + size], preferred_element_type=F32)
        hidden[:, c : c + size] = (a / (1.0 + jnp.exp(-a)) * b).astype(BF16)

    def lower(h, j):
        return jnp.dot(hidden[...], down[:, columns(h, j, 256)], preferred_element_type=F32)

    for j in range(2):
        pair_out[j] = lower(1 - core, j).astype(BF16)
        push(pair_out.at[j], pair_in.at[j], PAIR_BACK, (ep, partner))
    mine = [lower(core, j) for j in range(2)]
    landed(pair_in, PAIR_BACK, recv_sem)
    for j in range(2):
        out = mine[j] + pair_in[j].astype(F32)
        for i in range(2):
            store_rows(2 * j + i, out[:, 128 * i : 128 * i + 128])
    back[...] = wide[...].astype(BF16).reshape(n_ep, 8, 128)
    for k, p in enumerate(sources):
        push(back.at[k], back_in.at[ep], BACK, (p, tp))
    back_in[ep] = back[n_ep - 1]

    landed(back_in.at[pl.ds(0, n_ep - 1)], BACK, recv_sem)
    wide[...] = back_in[...].astype(F32).reshape(n_ep * 8, 128)
    picked = jnp.concatenate([read_rows(j) for j in range(4)], axis=1).astype(BF16)
    fin[...] = (
        jnp.dot(gather_high, picked, preferred_element_type=F32)
        + jnp.dot(gather_rest, picked, preferred_element_type=F32)
    ).astype(BF16)
    for i in range(1, n_tp):
        push(fin, fin_in.at[tp], LAST, (ep, lax.rem(tp + i, n_tp)))
    fin_in[tp] = fin[...]

    landed(res_other, RESIDUAL, recv_sem)
    landed(part_in.at[pl.ds(0, n_tp - 1)], PARTS, send_sem)
    landed(res_mine, RESIDUAL, send_sem)
    landed(disp.at[far_slots], FAR, send_sem)
    landed(disp.at[pl.ds(0, far - 1)], NEAR, send_sem)
    landed(disp_in.at[near_slots], PAIR_NEAR, send_sem)
    landed(disp_in.at[far_slots], PAIR_FAR, send_sem)
    landed(pair_out, PAIR_BACK, send_sem)
    landed(back.at[pl.ds(0, n_ep - 1)], BACK, send_sem)
    landed(fin_in.at[pl.ds(0, n_tp - 1)], LAST, recv_sem)
    for h in range(2):
        kept = jnp.where(core == h, res_mine[...].astype(F32), res_other[...].astype(F32))
        moved = fin_in[h].astype(F32)
        for t in range(2 + h, n_tp, 2):
            moved = moved + fin_in[t].astype(F32)
        mixed_o[:, half_width * h : half_width * (h + 1)] = (kept + moved).astype(BF16)
    landed(fin_in.at[pl.ds(0, n_tp - 1)], LAST, send_sem)


def write_out(*refs):
    ins, outs, sems = refs[:3], refs[3:6], refs[6]
    copies = [pltpu.make_async_copy(ins[i], outs[i], sems.at[i]) for i in range(3)]
    for copy in copies:
        copy.start()
    for copy in copies:
        copy.wait()


def solution(mesh):
    n_ep, n_tp = mesh.shape["ep"], mesh.shape["tp"]

    def body(*args):
        (tokens, attn_gain, w_query, w_key, w_value, attn_bias, key_cache, value_cache, lengths, w_out,
         ffn_gain, routes, route_weight, expert_gate, expert_up, expert_down) = args
        seqs, width = tokens.shape
        units = expert_gate.shape[2]
        half = width // 2
        operands = (
            tokens, attn_gain.reshape(1, width), w_query, w_key.T, w_value.T, attn_bias, key_cache, value_cache, lengths,
            w_out, ffn_gain.reshape(1, width), routes.T, route_weight.T, expert_gate, expert_up, expert_down,
        )
        vmem, smem = pltpu.VMEM, pltpu.SMEM

        def run(*refs):
            kernel(n_ep, n_tp, *refs)

        results = pl.pallas_call(
            run,
            name="layer",
            out_shape=(
                jax.ShapeDtypeStruct(tokens.shape, BF16),
                jax.ShapeDtypeStruct((seqs, w_key.shape[1]), BF16),
                jax.ShapeDtypeStruct((seqs, w_value.shape[1]), BF16),
            ),
            in_specs=[pl.BlockSpec(memory_space=pltpu.HBM)] * len(operands),
            out_specs=(pl.BlockSpec(memory_space=vmem),) * 3,
            scratch_shapes=[
                vmem(tokens.shape, BF16), vmem((1, width), F32), vmem(w_query.shape, BF16), vmem(w_key.shape[::-1], BF16),
                vmem(w_value.shape[::-1], BF16), smem(attn_bias.shape, F32), vmem(key_cache.shape, BF16),
                vmem(value_cache.shape, BF16), smem(lengths.shape, jnp.int32), vmem(w_out.shape, BF16),
                vmem((1, width), F32), vmem(routes.shape[::-1], jnp.int32), vmem(route_weight.shape[::-1], F32),
                vmem(expert_gate.shape[1:], BF16), vmem(expert_up.shape[1:], BF16), vmem(expert_down.shape[1:], BF16),
                vmem((512, 256), BF16), vmem((4 * seqs, 1024), F32), vmem((32 * seqs, 512), BF16), vmem((2, seqs, half), BF16),
                vmem((n_tp, seqs, half), BF16), *[vmem((n_ep, 8, 128), BF16)] * 5,
                *[vmem((2, 2 * n_ep, half // 2), BF16)] * 2, vmem((seqs, half), BF16),
                vmem((n_tp, seqs, half), BF16), *[vmem((seqs, half), BF16)] * 2, vmem((n_ep * 8, 128), F32),
                vmem((2 * n_ep, width), F32), vmem((2 * n_ep, width), BF16), vmem((2 * n_ep, units), BF16),
                pltpu.SemaphoreType.DMA((20,)), pltpu.SemaphoreType.DMA((9,)), pltpu.SemaphoreType.DMA((9,)),
            ],
            compiler_params=pltpu.CompilerParams(
                collective_id=0, has_side_effects=True, vmem_limit_bytes=48 * 1024 * 1024
            ),
        )(*[pltpu.with_memory_space_constraint(x, pltpu.HBM) for x in operands])

        return pl.pallas_call(
            write_out,
            name="write_out",
            out_shape=tuple(pltpu.HBM(r.shape, r.dtype) for r in results),
            in_specs=[pl.BlockSpec(memory_space=vmem)] * 3,
            out_specs=(pl.BlockSpec(memory_space=pltpu.HBM),) * 3,
            scratch_shapes=[pltpu.SemaphoreType.DMA((3,))],
            compiler_params=pltpu.CompilerParams(vmem_limit_bytes=1024 * 1024),
        )(*[pltpu.with_memory_space_constraint(r, vmem) for r in results])

    return jax.shard_map(
        body,
        mesh=mesh,
        in_specs=(
            P("ep", None), P(), P(None, "tp"), P(None, "tp"), P(None, "tp"), P("tp"), P("ep", "tp", None),
            P("ep", "tp", None), P("ep"), P("tp", None), P(), P("ep", None), P("ep", None), P("ep", None, "tp"),
            P("ep", None, "tp"), P("ep", "tp", None),
        ),
        out_specs=(P("ep", None), P("ep", "tp"), P("ep", "tp")),
        check_vma=False,
    )
```
